1024 devices in a mesh: ep: 32 (over z, core), tp: 32 (over y, x).
Axes of the slice: x: 4, y: 8, z: 16, core: 2. Of those that a mesh axis runs over, the one named last changes fastest.
Arguments:
- tokens: bfloat16 [8192, 2048], P('ep'), may hold values from -6 to 6
- gate_proj: bfloat16 [32, 2048, 4096], P('ep', None, 'tp'), may hold values from -0.125 to 0.125
- up_proj: bfloat16 [32, 2048, 4096], P('ep', None, 'tp'), may hold values from -0.125 to 0.125
- down_proj: bfloat16 [32, 4096, 2048], P('ep', 'tp'), may hold values from -0.09375 to 0.09375
- side_input_weight: bfloat16 [2048, 1024], P(None, 'tp'), may hold values from -0.125 to 0.125
- dense_out: bfloat16 [1024, 2048], P(None, 'tp'), may hold values from -0.1875 to 0.1875
- dense_gate: bfloat16 [2048], replicated, may hold values from -0.125 to 0.125
- chosen_rows: int32 [32, 1024], P(None, 'ep'), may hold values from 0 to 255, as said below
- choice_weights: float32 [32, 1024], P(None, 'ep'), may hold values from 0.25 to 1
Outputs:
- mixed: bfloat16 [8192, 2048], P('ep', 'tp')
The draws below stay inside these ranges and needn't reach their ends.
Inputs may be any that keep to these rules, and one draw needn't show every extreme that they name: `chosen_rows`: for each expert and each block of 32 columns (one index of ep), the 32 rows are distinct rows of that index's 256 tokens; every expert reads exactly 32 tokens of every index.
All inputs are finite; a program needn't handle non-finite values.
Results may differ from the reference program's by a relative error of at most 0.015.
Values may be sent and summed in bfloat16 or wider, within the bound.
A program may use at most 64 MiB of HBM per device.

```python
import jax
import jax.numpy as jnp
from jax import lax

D = 2048
FF = 4096
DENSE_FF = 1024
TOK_DEV = 256
SLOT = 32
EXPERTS = 32
CAP = 1024
TOKENS = 8192
N_TP = 32


def draw_chosen_rows(key, part):
    block_list = TOKENS // TOK_DEV
    keys = jax.random.split(jax.random.fold_in(key, 17), EXPERTS * block_list)
    orders = jax.vmap(lambda k: jax.random.permutation(k, TOK_DEV))(keys)
    picked = orders[:, :SLOT].astype(jnp.int32)
    return picked.reshape(EXPERTS, block_list * SLOT)


def level_of(stream_key, extent, shards, least, largest):
    def one(axis_at, parts):
        draws = jax.random.uniform(jax.random.fold_in(jax.random.fold_in(stream_key, 6), axis_at), (parts,), jnp.float32, least / len(shards), largest / len(shards))
        return jnp.repeat(jnp.exp(draws), extent[axis_at] // parts).reshape((-1,) + (1,) * (len(extent) - axis_at - 1))

    level = one(*shards[0])
    for cut in shards[1:]:
        level = level * one(*cut)
    return level


def gaussian(rng, dims, width, bound, cuts=(), dtype=jnp.bfloat16):
    factor_of = level_of(rng, dims, cuts, -0.22, 0.18) if cuts else 1.0
    values = jax.random.normal(rng, dims, jnp.float32) * width * factor_of
    return jnp.minimum(jnp.maximum(values, -bound), bound).astype(dtype)


def setup_inputs(seed: int = 0) -> dict:
    splits = jax.random.split(jax.random.key(seed), 10)
    return {
        "tokens": gaussian(splits[0], (TOKENS, D), 1.0, 6.0, ((0, 32),)),
        "gate_proj": gaussian(splits[1], (EXPERTS, D, FF), D ** -0.5, 0.125, ((0, 32), (2, 32))),
        "up_proj": gaussian(splits[2], (EXPERTS, D, FF), D ** -0.5, 0.125, ((0, 32), (2, 32))),
        "down_proj": gaussian(splits[3], (EXPERTS, FF, D), FF ** -0.5, 0.09375, ((0, 32), (1, 32))),
        "side_input_weight": gaussian(splits[4], (D, DENSE_FF), D ** -0.5, 0.125, ((1, 32),)),
        "dense_out": gaussian(splits[5], (DENSE_FF, D), DENSE_FF ** -0.5, 0.1875, ((1, 32),)),
        "dense_gate": gaussian(splits[6], (D,), D ** -0.5, 0.125),
        "chosen_rows": draw_chosen_rows(jax.random.fold_in(splits[9], 71), 0),
        "choice_weights": jnp.clip(0.25 + 0.75 * jax.random.uniform(splits[8], (EXPERTS, CAP), jnp.float32) ** level_of(splits[8], (EXPERTS, CAP), ((1, 32),), -0.2, 0.2), 0.25, 1.0),
    }


def reference(tokens, gate_proj, up_proj, down_proj, side_input_weight, dense_out, dense_gate, chosen_rows, choice_weights):
    token_id = ((jnp.arange(CAP) // SLOT) * TOK_DEV).astype(jnp.int32)[None, :] + chosen_rows.astype(jnp.int32)

    def one_expert(routed, inputs):
        w_gate, w_up, w_down, ids, weights = inputs
        picked = jnp.take(tokens, ids, axis=0)
        gate_val = jnp.dot(picked, w_gate, preferred_element_type=jnp.float32)
        up_val = jnp.dot(picked, w_up, preferred_element_type=jnp.float32)
        hidden = (jax.nn.silu(gate_val) * up_val).astype(jnp.bfloat16)
        block_list = hidden.reshape(CAP, N_TP, FF // N_TP).astype(jnp.float32)
        down_weight_blocks = w_down.reshape(N_TP, FF // N_TP, D).astype(jnp.float32)
        part = jnp.einsum('lyk,yka->yla', block_list, down_weight_blocks, precision=lax.Precision.HIGHEST)
        part = lax.optimization_barrier(part.astype(jnp.bfloat16)).astype(jnp.float32)
        expert_out = jnp.sum(part, axis=0).astype(jnp.bfloat16)
        routed = routed.at[ids].add(weights[:, None] * expert_out.astype(jnp.float32))
        return routed, None

    routed, _ = lax.scan(one_expert, jnp.zeros((TOKENS, D), jnp.float32),
                         (gate_proj, up_proj, down_proj, token_id, choice_weights))
    dense_hidden = jax.nn.silu(jnp.dot(tokens, side_input_weight, preferred_element_type=jnp.float32)).astype(jnp.bfloat16)
    dense_val = jnp.dot(dense_hidden, dense_out, preferred_element_type=jnp.float32)
    side_gate = jax.nn.sigmoid(jnp.dot(tokens, dense_gate, preferred_element_type=jnp.float32))
    return (routed + side_gate[:, None] * dense_val).astype(jnp.bfloat16)
```

```python
import functools

import jax
import jax.numpy as jnp
from jax import lax
from jax.experimental import pallas as pl
from jax.experimental.pallas import tpu as pltpu
from jax.sharding import Mesh
from jax.sharding import PartitionSpec as P

MESH = pl.DeviceIdType.MESH
F32 = jnp.float32
BF16 = jnp.bfloat16
C = 128
NX = 4


def kernel(
    cfg,
    tok_hbm, gate_hbm, up_hbm, down_hbm, side_hbm, dout_hbm, dgate_ref, rows_ref, wts_ref,
    out_ref,
    tok, side, dout, w1, wd, sel, xbuf, part, m_hi, m_lo, dh,
    na, nb, nxr, fxr, fa, fb, fin, ret, exch_out, exch_in,
    loc_sem, z_ss, z_rs, w_ss, w_rs, n_ss, n_rs, f_ss, f_rs, d_ss, d_rs,
    rn_ss, rn_rs, rf_ss, rf_rs, r_ss, r_rs, e_ss, e_rs,
):
    NZ, NY, SLOT, NEAR = cfg
    LONG, SHORT = NY // 2, NY // 2 - 1
    NR = NEAR * SLOT
    ROWS = NZ * SLOT
    FR = ROWS - NR
    D = tok.shape[1]

    z, c, y, x = (lax.axis_index(a) for a in ("z", "c", "y", "x"))
    q = x // 2
    xn = NX - 1 - x
    xp = x + 1 - 2 * (x % 2)
    g = ((x + 1) // 2) % 2
    holder = c == g
    sgn = 1 - 2 * c

    def yy(j):
        return lax.rem(y + sgn * j + 2 * NY, NY)

    def zz(j):
        return lax.rem(z + j + 2 * NZ, NZ)

    def z_off(i):
        return ((i + 1) // 2) * (1 - 2 * (i % 2))

    def col(yv, qv):
        return pl.ds(pl.multiple_of(yv * 2 * C + qv * C, C), C)

    def col2(yv):
        return pl.ds(pl.multiple_of(yv * 2 * C, 2 * C), 2 * C)

    near, far = pl.ds(0, NR), pl.ds(NR, FR)
    toA, toB = {"y": yy(1)}, {"y": yy(-1)}
    toN, toP, toS = {"x": xn}, {"x": xp}, {"c": 1 - c}

    def rc(src, dst, ss, rs, dev):
        return pltpu.make_async_remote_copy(
            src_ref=src, dst_ref=dst, send_sem=ss, recv_sem=rs, device_id=dev, device_id_type=MESH
        )

    sent = []

    def send(src, dst, ss, rs, dev):
        cp = rc(src, dst, ss, rs, dev)
        cp.start()
        sent.append(cp)

    def arrive(dst, ss, rs):
        rc(dst, dst, ss, rs, toS).wait_recv()

    barrier = pltpu.get_barrier_semaphore()
    for dev in (toA, toB, toN, toP, toS):
        pl.semaphore_signal(barrier, inc=1, device_id=dev, device_id_type=MESH)

    @pl.loop(1, NZ)
    def _(k):
        pl.semaphore_signal(barrier, inc=1, device_id={"z": zz(k)}, device_id_type=MESH)

    l_tok = pltpu.make_async_copy(tok_hbm, tok, loc_sem.at[0])
    l_side = pltpu.make_async_copy(side_hbm, side, loc_sem.at[1])
    l_dout = pltpu.make_async_copy(dout_hbm, dout, loc_sem.at[2])
    l_tok.start()
    l_side.start()
    l_dout.start()
    own_w = (gate_hbm.at[0], up_hbm.at[0], down_hbm.at[0])

    def w_dst(b):
        return (w1.at[b, :, pl.ds(0, C)], w1.at[b, :, pl.ds(C, C)], wd.at[b])

    @pl.when(holder)
    def _():
        for i in range(3):
            pltpu.make_async_copy(own_w[i], w_dst(0)[i], w_rs.at[i]).start()

    ids = rows_ref[pl.ds(g, 1), :]
    hit = lax.broadcasted_iota(jnp.int32, (tok.shape[0], ROWS), 0) == ids
    l_tok.wait()
    picked = lax.dot_general(
        jnp.where(hit, 1.0, 0.0).astype(BF16), tok[:, col(y, q)], (((0,), (0,)), ((), ())),
        preferred_element_type=F32,
    )
    sel[...] = picked.astype(BF16).reshape(NZ, SLOT, C)
    wts = wts_ref[pl.ds(g, 1), :]
    w_hi = wts.astype(BF16).astype(F32)
    w_lo = wts - w_hi
    m_hi[...] = jnp.where(hit, w_hi, 0.0).astype(BF16)
    m_lo[...] = jnp.where(hit, w_lo, 0.0).astype(BF16)

    l_side.wait()
    dpre = jnp.dot(tok[...], side[...], preferred_element_type=F32)
    dpre = dpre * (1.0 / (1.0 + jnp.exp(-dpre)))
    dh[x, y] = dpre.T.astype(BF16)

    pl.semaphore_wait(barrier, 5 + NZ - 1)

    @pl.loop(1, NZ)
    def _(i):
        dest = zz(z_off(i))
        rc(
            sel.at[dest], xbuf.at[pl.ds(pl.multiple_of(i * SLOT, SLOT), SLOT), col(y, q)],
            z_ss.at[i], z_rs.at[i], {"z": dest},
        ).start()

    xbuf[pl.ds(0, SLOT), col(y, q)] = sel[z]

    @pl.when(holder)
    def _():
        for i in range(3):
            rc(own_w[i], w_dst(0)[i], w_ss.at[i], w_rs.at[i], toS).start()

    @pl.when(jnp.logical_not(holder))
    def _():
        for i in range(3):
            rc(own_w[i], w_dst(1)[i], w_ss.at[i], w_rs.at[3 + i], toP).start()

    def z_arrive(lo, hi):
        @pl.loop(lo, hi)
        def _(i):
            arrive(
                xbuf.at[pl.ds(pl.multiple_of(i * SLOT, SLOT), SLOT), col(y, q)],
                z_ss.at[i], z_rs.at[i],
            )

    z_arrive(1, NEAR)
    blk = xbuf.at[near, col(y, q)]
    send(blk, blk, n_ss.at[0], n_rs.at[0], toN)
    arrive(xbuf.at[near, col(y, 1 - q)], n_ss.at[0], n_rs.at[0])

    def n_send(yv, way, s):
        blk = xbuf.at[near, col2(yv)]
        k = 1 + way * LONG + s
        dev = toB if way else toA
        send(blk, blk, n_ss.at[k], n_rs.at[k], dev)
        send(dh.at[x, yv], dh.at[x, yv], d_ss.at[k], d_rs.at[k], dev)

    def n_arrive(yv, way, s):
        blk = xbuf.at[near, col2(yv)]
        k = 1 + way * LONG + s
        arrive(blk, n_ss.at[k], n_rs.at[k])
        arrive(dh.at[x, yv], d_ss.at[k], d_rs.at[k])

    n_send(y, 0, 0)
    n_send(y, 1, 0)

    def f_send(yv, way, s):
        blk = xbuf.at[far, col(yv, q)]
        k = way * LONG + s
        send(blk, blk, f_ss.at[k], f_rs.at[k], toB if way else toA)

    def f_arrive(yv, way, s):
        k = way * LONG + s
        arrive(xbuf.at[far, col(yv, q)], f_ss.at[k], f_rs.at[k])

    def fx_send(yv, k):
        blk = xbuf.at[far, col(yv, q)]
        send(blk, blk, f_ss.at[NY + k], f_rs.at[NY + k], toN)

    def fx_arrive(yv, k):
        arrive(xbuf.at[far, col(yv, 1 - q)], f_ss.at[NY + k], f_rs.at[NY + k])

    z_arrive(NEAR, NZ)
    f_send(y, 0, 0)
    f_send(y, 1, 0)
    fx_send(y, 0)
    for s in range(1, LONG + 1):
        ya, yb = yy(-s), yy(s)
        n_arrive(ya, 0, s - 1)
        if s < LONG:
            n_send(ya, 0, s)
        if s <= SHORT:
            n_arrive(yb, 1, s - 1)
            if s < SHORT:
                n_send(yb, 1, s)
        f_arrive(ya, 0, s - 1)
        if s < LONG:
            f_send(ya, 0, s)
        fx_send(ya, s)
        if s <= SHORT:
            f_arrive(yb, 1, s - 1)
            if s < SHORT:
                f_send(yb, 1, s)
            fx_send(yb, LONG + s)
    send(dh.at[x], dh.at[x], d_ss.at[0], d_rs.at[0], toN)

    @pl.when(holder)
    def _():
        for i in range(3):
            pltpu.make_async_copy(own_w[i], w_dst(0)[i], w_rs.at[i]).wait()
        for i in range(3):
            arrive(w_dst(1)[i], w_ss.at[i], w_rs.at[3 + i])
            rc(w_dst(1)[i], w_dst(1)[i], w_ss.at[3 + i], w_rs.at[3 + i], toS).start()

    @pl.when(jnp.logical_not(holder))
    def _():
        for i in range(3):
            arrive(w_dst(0)[i], w_ss.at[i], w_rs.at[i])
            arrive(w_dst(1)[i], w_ss.at[i], w_rs.at[3 + i])

    def experts(rows):
        halves = []
        for b in range(2):
            gu = jnp.dot(xbuf[rows, :], w1[b], preferred_element_type=F32)
            gv, uv = gu[:, :C], gu[:, C:]
            halves.append((gv * (1.0 / (1.0 + jnp.exp(-gv))) * uv).astype(BF16))
        hidden = jnp.concatenate(halves, axis=1)
        width = 512
        for n in range(D // width):
            cols = pl.ds(n * width, width)
            wdn = wd[:, :, cols].reshape(2 * C, width)
            part[rows, cols] = jnp.dot(hidden, wdn, preferred_element_type=F32).astype(BF16)

    def add(*terms):
        total = terms[0].astype(F32)
        for t in terms[1:]:
            total = total + t.astype(F32)
        return total.astype(BF16)

    experts(near)

    def rn_send(src, way, s):
        k = 1 + way * LONG + s
        dst = nb.at[s] if way else na.at[s]
        send(src, dst, rn_ss.at[k], rn_rs.at[k], toB if way else toA)

    def rn_arrive(way, s):
        k = 1 + way * LONG + s
        arrive(nb.at[s] if way else na.at[s], rn_ss.at[k], rn_rs.at[k])

    rn_send(part.at[near, col2(yy(LONG))], 0, 0)
    rn_send(part.at[near, col2(yy(-SHORT))], 1, 0)

    for k in range(NY):
        fx_arrive(yy(-k) if k <= LONG else yy(k - LONG), k)
    experts(far)

    def rx_index(j):
        return j if j >= 0 else LONG - j

    order = [LONG]
    for j in range(SHORT, 0, -1):
        order += [-j, j]
    order += [0]
    for j in order:
        k = rx_index(j)
        send(part.at[far, col(yy(j), 1 - q)], fxr.at[k], rf_ss.at[NY + k], rf_rs.at[NY + k], toN)

    def rf_send(src, way, s):
        k = way * LONG + s
        dst = fb.at[s] if way else fa.at[s]
        send(src, dst, rf_ss.at[k], rf_rs.at[k], toB if way else toA)

    def rf_arrive(way, s):
        k = way * LONG + s
        arrive(fb.at[s] if way else fa.at[s], rf_ss.at[k], rf_rs.at[k])

    def rx_arrive(j):
        k = rx_index(j)
        arrive(fxr.at[k], rf_ss.at[NY + k], rf_rs.at[NY + k])
        return fxr[k], part[far, col(yy(j), q)]

    fxr[LONG] = add(*rx_arrive(LONG))
    rf_send(fxr.at[LONG], 0, 0)
    fxr[LONG + SHORT] = add(*rx_arrive(-SHORT))
    rf_send(fxr.at[LONG + SHORT], 1, 0)

    for s in range(1, LONG):
        rn_arrive(0, s - 1)
        na[s - 1] = add(na[s - 1], part[near, col2(yy(LONG - s))])
        rn_send(na.at[s - 1], 0, s)
        if s < SHORT:
            rn_arrive(1, s - 1)
            nb[s - 1] = add(nb[s - 1], part[near, col2(yy(s - SHORT))])
            rn_send(nb.at[s - 1], 1, s)
        rf_arrive(0, s - 1)
        fa[s - 1] = add(fa[s - 1], *rx_arrive(LONG - s))
        rf_send(fa.at[s - 1], 0, s)
        if s < SHORT:
            rf_arrive(1, s - 1)
            fb[s - 1] = add(fb[s - 1], *rx_arrive(s - SHORT))
            rf_send(fb.at[s - 1], 1, s)

    rn_arrive(0, LONG - 1)
    rn_arrive(1, SHORT - 1)
    na[LONG - 1] = add(na[LONG - 1], nb[SHORT - 1], part[near, col2(y)])
    send(
        na.at[LONG - 1, :, pl.ds(pl.multiple_of((1 - q) * C, C), C)], nxr, rn_ss.at[0], rn_rs.at[0], toN
    )
    rf_arrive(0, LONG - 1)
    rf_arrive(1, SHORT - 1)
    fin[far, :] = add(fa[LONG - 1], fb[SHORT - 1], *rx_arrive(0))

    def z_return(lo, hi):
        @pl.loop(lo, hi)
        def _(i):
            rc(
                fin.at[pl.ds(pl.multiple_of(i * SLOT, SLOT), SLOT), :], ret.at[z],
                r_ss.at[i], r_rs.at[i], {"z": zz(-z_off(i))},
            ).start()

    z_return(NEAR, NZ)
    arrive(nxr, rn_ss.at[0], rn_rs.at[0])
    mine = na[LONG - 1, :, pl.ds(pl.multiple_of(q * C, C), C)]
    fin[near, :] = add(mine, nxr[...])
    z_return(1, NEAR)
    ret[z] = fin[pl.ds(0, SLOT), :]

    arrive(dh.at[xn], d_ss.at[0], d_rs.at[0])
    send(dh.at[x], dh.at[x], d_ss.at[NY], d_rs.at[NY], toP)
    send(dh.at[xn], dh.at[xn], d_ss.at[NY + 1], d_rs.at[NY + 1], toP)
    arrive(dh.at[xp], d_ss.at[NY], d_rs.at[NY])
    arrive(dh.at[NX - 1 - xp], d_ss.at[NY + 1], d_rs.at[NY + 1])
    l_dout.wait()
    dense = None
    for xv in range(NX):
        term = lax.dot_general(
            dh[xv].reshape(NY * 32, tok.shape[0]), dout[:, xv].reshape(NY * 32, 64),
            (((0,), (0,)), ((), ())), preferred_element_type=F32,
        )
        dense = term if dense is None else dense + term
    logit = jnp.sum(tok[...].astype(F32) * dgate_ref[...].astype(F32), axis=1, keepdims=True)
    dense = dense * (1.0 / (1.0 + jnp.exp(-logit)))

    @pl.loop(1, NZ)
    def _(i):
        arrive(ret.at[zz(z_off(i))], r_ss.at[i], r_rs.at[i])

    back = ret[...].reshape(ROWS, C)
    routed = jnp.dot(m_hi[...], back, preferred_element_type=F32) + jnp.dot(
        m_lo[...], back, preferred_element_type=F32
    )
    exch_out[...] = routed.astype(BF16)
    send(exch_out, exch_in, e_ss, e_rs, toP)
    arrive(exch_in, e_ss, e_rs)
    total = routed + exch_in[...].astype(F32)
    total = jnp.where(x % 2 == 1, pltpu.roll(total, C // 2, 1), total)
    out_ref[...] = (total[:, : C // 2] + dense).astype(BF16)

    for cp in sent:
        cp.wait_send()

    @pl.loop(1, NZ)
    def _(i):
        rc(sel.at[0], sel.at[0], z_ss.at[i], z_rs.at[i], toS).wait_send()
        rc(ret.at[0], ret.at[0], r_ss.at[i], r_rs.at[i], toS).wait_send()

    for i in range(3):
        rc(own_w[i], w_dst(0)[i], w_ss.at[i], w_rs.at[i], toS).wait_send()

    @pl.when(holder)
    def _():
        for i in range(3):
            rc(w_dst(1)[i], w_dst(1)[i], w_ss.at[3 + i], w_rs.at[3 + i], toS).wait_send()


def per_device(sizes, near, tokens, gate, up, down, side, dout, dgate, rows, wts):
    NZ, NY = sizes
    T, D = tokens.shape
    slot = rows.shape[1]
    n_rows = NZ * slot
    NR = near * slot
    FR = n_rows - NR
    LONG, SHORT = NY // 2, NY // 2 - 1

    def by_group(a):
        return a.reshape(NZ, 2, slot).transpose(1, 0, 2).reshape(2, n_rows)

    any_ = pl.BlockSpec(memory_space=pl.ANY)
    vmem = pl.BlockSpec(memory_space=pltpu.VMEM)
    dma = pltpu.SemaphoreType.DMA
    return pl.pallas_call(
        functools.partial(kernel, (NZ, NY, slot, near)),
        out_shape=jax.ShapeDtypeStruct((T, 64), BF16),
        in_specs=[any_] * 6 + [vmem] * 3,
        out_specs=vmem,
        scratch_shapes=[
            pltpu.VMEM((T, D), BF16),
            pltpu.VMEM((D, 32), BF16),
            pltpu.VMEM((NY, NX, 32, 64), BF16),
            pltpu.VMEM((2, D, 2 * C), BF16),
            pltpu.VMEM((2, C, D), BF16),
            pltpu.VMEM((NZ, slot, C), BF16),
            pltpu.VMEM((n_rows, D), BF16),
            pltpu.VMEM((n_rows, D), BF16),
            pltpu.VMEM((T, n_rows), BF16),
            pltpu.VMEM((T, n_rows), BF16),
            pltpu.VMEM((NX, NY, 32, T), BF16),
            pltpu.VMEM((LONG, NR, 2 * C), BF16),
            pltpu.VMEM((SHORT, NR, 2 * C), BF16),
            pltpu.VMEM((NR, C), BF16),
            pltpu.VMEM((NY, FR, C), BF16),
            pltpu.VMEM((LONG, FR, C), BF16),
            pltpu.VMEM((SHORT, FR, C), BF16),
            pltpu.VMEM((n_rows, C), BF16),
            pltpu.VMEM((NZ, slot, C), BF16),
            pltpu.VMEM((T, C), BF16),
            pltpu.VMEM((T, C), BF16),
            dma((3,)),
            dma((NZ,)), dma((NZ,)),
            dma((6,)), dma((6,)),
            dma((NY,)), dma((NY,)),
            dma((2 * NY,)), dma((2 * NY,)),
            dma((NY + 2,)), dma((NY + 2,)),
            dma((NY,)), dma((NY,)),
            dma((2 * NY,)), dma((2 * NY,)),
            dma((NZ,)), dma((NZ,)),
            dma, dma,
        ],
        compiler_params=pltpu.CompilerParams(
            collective_id=0, has_side_effects=True, vmem_limit_bytes=60 * 1024 * 1024
        ),
        name="layer",
    )(
        tokens, gate, up, down, side, dout.reshape(NY, NX, 32, 64), dgate.reshape(1, D),
        by_group(rows), by_group(wts),
    )


def solution(mesh, sizes=(16, 8), near=7):
    NZ, NY = sizes
    torus = Mesh(mesh.devices.reshape(NZ, 2, NY, NX), ("z", "c", "y", "x"))
    EP, TP = ("z", "c"), ("y", "x")
    return jax.shard_map(
        functools.partial(per_device, sizes, near),
        mesh=torus,
        in_specs=(
            P(EP, None),
            P(EP, None, TP),
            P(EP, None, TP),
            P(EP, TP, None),
            P(None, TP),
            P(None, TP),
            P(),
            P(None, EP),
            P(None, EP),
        ),
        out_specs=P(EP, TP),
        check_vma=False,
    )
```

```python
import functools

import jax
import jax.numpy as jnp
from jax import lax
from jax.experimental import pallas as pl
from jax.experimental.pallas import tpu as pltpu
from jax.sharding import Mesh
from jax.sharding import PartitionSpec as P

MESH = pl.DeviceIdType.MESH
F32 = jnp.float32
BF16 = jnp.bfloat16
C = 128
NX = 4


def kernel(
    cfg,
    tok_hbm, gate_hbm, up_hbm, down_hbm, side_hbm, dout_hbm, dgate_ref, rows_ref, wts_ref,
    out_ref,
    tok, side, dout, w1, wd, sel, sel_whole, xbuf, part, hits, m_hi, m_lo, dh, sel_far, bundle,
    na, nb, nxr, fxr, fa, fb, fin, ret, exch_out, exch_in, side_gate,
    loc_sem, l_ss, l_rs, m_ss, z_ss, z_rs, w_ss, w_rs, n_ss, n_rs, f_ss, f_rs, d_ss, d_rs,
    rn_ss, rn_rs, rf_ss, rf_rs, r_ss, r_rs, e_ss, e_rs,
):
    NZ, NY, SLOT, DIRECT, PAIRED, NEAR = cfg
    LONG, SHORT = NY // 2, NY // 2 - 1
    ROWS = NZ * SLOT
    NR, FR = 2 * NEAR * SLOT, 2 * (NZ - NEAR) * SLOT
    T, D = tok.shape

    z, c, y, x = (lax.axis_index(a) for a in ("z", "c", "y", "x"))
    q = x // 2
    xn = NX - 1 - x
    xp = x + 1 - 2 * (x % 2)
    g = ((x + 1) // 2) % 2
    hub = c == 1
    REACH = NZ // 4
    sgn = 1 - 2 * c

    def yy(j):
        return lax.rem(y + sgn * j + 2 * NY, NY)

    def zz(j):
        return lax.rem(z + j + 2 * NZ, NZ)

    def z_off(i):
        return ((i + 1) // 2) * (1 - 2 * (i % 2))

    def col(yv, qv):
        return pl.ds(pl.multiple_of(yv * 2 * C + qv * C, C), C)

    def col2(yv):
        return pl.ds(pl.multiple_of(yv * 2 * C, 2 * C), 2 * C)

    near, far = pl.ds(0, NR), pl.ds(NR, FR)
    pair_rows = pl.ds(2 * DIRECT * SLOT, 2 * (PAIRED - DIRECT) * SLOT)
    one_rows = pl.ds(2 * PAIRED * SLOT, 2 * (NZ - PAIRED) * SLOT)
    toA, toB = {"y": yy(1)}, {"y": yy(-1)}
    toN, toP, toS = {"x": xn}, {"x": xp}, {"c": 1 - c}

    def rc(src, dst, ss, rs, dev):
        return pltpu.make_async_remote_copy(
            src_ref=src, dst_ref=dst, send_sem=ss, recv_sem=rs, device_id=dev, device_id_type=MESH
        )

    sent, mine = [], []

    def send(kept, src, dst, ss, rs, dev):
        cp = rc(src, dst, ss, rs, dev)
        cp.start()
        kept.append(cp)

    def arrive(dst, ss, rs):
        rc(dst, dst, ss, rs, toS).wait_recv()

    barrier = pltpu.get_barrier_semaphore()

    def greet(dev):
        pl.semaphore_signal(barrier, inc=1, device_id=dev, device_id_type=MESH)

    for dev in (toA, toB, toN, toP, toS):
        greet(dev)

    @pl.loop(1, REACH + 1)
    def _(k):
        greet({"z": zz(k), "c": 1})
        greet({"z": zz(-k), "c": 1})

    @pl.when(hub)
    def _():
        greet({"x": xp, "c": 0})

        @pl.loop(1, REACH + 1)
        def _(k):
            greet({"z": zz(k), "c": 0})
            greet({"z": zz(-k), "c": 0})

    l_tok = pltpu.make_async_copy(tok_hbm, tok, loc_sem.at[0])
    l_side = pltpu.make_async_copy(side_hbm, side, loc_sem.at[1])
    l_dout = pltpu.make_async_copy(dout_hbm, dout, loc_sem.at[2])
    l_tok.start()
    l_side.start()
    l_dout.start()
    own_w = (gate_hbm.at[0], up_hbm.at[0], down_hbm.at[0])

    def w_dst(b):
        return (w1.at[b, :, pl.ds(0, C)], w1.at[b, :, pl.ds(C, C)], wd.at[b])

    @pl.when(jnp.logical_and(hub, g == 1))
    def _():
        for i in range(3):
            pltpu.make_async_copy(own_w[i], w_dst(0)[i], w_rs.at[i]).start()

    ids = rows_ref[pl.ds(g, NZ, stride=2), :].T
    token = lax.broadcasted_iota(jnp.int32, (SLOT, T), 1)
    for k in range(NZ):
        hits[pl.ds(k * SLOT, SLOT), :] = jnp.where(ids[:, k : k + 1] == token, 1.0, 0.0).astype(BF16)
    l_tok.wait()
    picked = jnp.dot(hits[...], tok[:, col2(y)], preferred_element_type=F32)
    sel[...] = picked.astype(BF16).reshape(NZ, SLOT, 2 * C)
    own_chunk = pl.ds(pl.multiple_of(q * C, C), C)
    for d, way in enumerate((1, -1)):
        for j in range(REACH):
            sel_far[d, j] = sel[zz(way * (REACH + 1 + j)), :, own_chunk]

    @pl.when(hub)
    def _():
        pl.semaphore_wait(barrier, 5 + 4 * REACH)

    @pl.when(jnp.logical_not(hub))
    def _():
        pl.semaphore_wait(barrier, 6 + 2 * REACH)


    def slot_rows(i, core):
        return pl.ds(pl.multiple_of((2 * i + core) * SLOT, SLOT), SLOT)

    @pl.loop(DIRECT, PAIRED)
    def _(i):
        dest = zz(z_off(i))
        rc(
            sel.at[dest], xbuf.at[slot_rows(i, c), col2(y)], z_ss.at[i], z_rs.at[2 * i + c],
            {"z": dest, "c": 1},
        ).start()

    for d, way in enumerate((1, -1)):
        send(
            sent, sel_far.at[d], bundle.at[d, c], l_ss.at[d], l_rs.at[2 * d + c],
            {"z": zz(way * REACH), "c": 1},
        )

    def w_send(b, dev):
        for i in range(3):
            rc(own_w[i], w_dst(b)[i], w_ss.at[i], w_rs.at[3 * b + i], dev).start()

    keeps = g == c

    @pl.when(jnp.logical_not(keeps))
    def _():
        w_send(1, {"x": xp, "c": 1})

    @pl.when(jnp.logical_and(keeps, jnp.logical_not(hub)))
    def _():
        w_send(0, toS)

    l_side.wait()
    transposed = (((1,), (1,)), ((), ()))
    dpre = lax.dot_general(side[...], tok[...], transposed, preferred_element_type=F32)
    dh[y, x] = (dpre * (1.0 / (1.0 + jnp.exp(-dpre)))).astype(BF16)

    def d_send(kept, yv, way, s):
        k = 1 + way * LONG + s
        blk = dh.at[yv, x]
        send(kept, blk, blk, d_ss.at[k], d_rs.at[k], toB if way else toA)

    def d_step(s):
        for way, last in ((0, LONG), (1, SHORT)):
            if s < last:
                yv = yy(s + 1) if way else yy(-s - 1)
                k = 1 + way * LONG + s
                arrive(dh.at[yv, x], d_ss.at[k], d_rs.at[k])
                if s < last - 1:
                    d_send(mine, yv, way, s + 1)

    d_send(sent, y, 0, 0)
    d_send(sent, y, 1, 0)

    for i in range(DIRECT):
        block = hits[pl.ds(pl.multiple_of(zz(z_off(i)) * SLOT, SLOT), SLOT), :]
        sel_whole[i] = jnp.dot(block, tok[...], preferred_element_type=F32).astype(BF16)

    def whole_send():
        for i in range(1, DIRECT):
            dest = zz(z_off(i))
            rc(
                sel_whole.at[i], xbuf.at[slot_rows(i, c), :], z_ss.at[i], z_rs.at[2 * i + c],
                {"z": dest, "c": 1},
            ).start()

    def d_across():
        send(mine, dh.at[:, x], dh.at[:, x], d_ss.at[0], d_rs.at[0], toN)

    def d_pair():
        arrive(dh.at[:, xn], d_ss.at[0], d_rs.at[0])
        for k, xv in ((NY, x), (NY + 1, xn)):
            send(mine, dh.at[:, xv], dh.at[:, xv], d_ss.at[k], d_rs.at[k], toP)

    def weights_of_rows():
        wts = wts_ref[pl.ds(g, NZ, stride=2), :].T
        w_hi = wts.astype(BF16).astype(F32)
        w_lo = wts - w_hi
        for k in range(NZ):
            rows = pl.ds(k * SLOT, SLOT)
            hit = hits[rows, :].astype(F32)
            m_hi[rows, :] = (hit * w_hi[:, k : k + 1]).astype(BF16)
            m_lo[rows, :] = (hit * w_lo[:, k : k + 1]).astype(BF16)
        dgate = dgate_ref[...].astype(F32)
        dgate = jnp.concatenate([dgate[k : k + 1, :] for k in range(D // C)], axis=1).astype(BF16)
        logit = lax.dot_general(dgate, tok[...], transposed, preferred_element_type=F32)
        side_gate[...] = 1.0 / (1.0 + jnp.exp(-logit))

    @pl.when(jnp.logical_not(hub))
    def _():
        mine.clear()
        rc(
            sel_whole.at[0], xbuf.at[slot_rows(0, 0), :], z_ss.at[0], z_rs.at[0], toS
        ).start()
        d_step(0)
        d_step(1)
        whole_send()
        weights_of_rows()
        for s in range(2, LONG):
            d_step(s)
        d_across()
        d_pair()
        arrive(ret.at[z], r_ss.at[0], r_rs.at[0])
        for cp in mine:
            cp.wait_send()

    @pl.when(hub)
    def _():
        mine.clear()
        xbuf[slot_rows(0, 1), :] = sel_whole[0]
        for d, way in enumerate((1, -1)):
            for core in range(2):
                arrive(bundle.at[d, core], l_ss.at[d], l_rs.at[2 * d + core])
                for j in range(REACH):
                    k = REACH + 1 + j
                    if 2 * k == NZ and d != core:
                        continue
                    i = 2 * k - 1 if d else min(2 * k, NZ - 1)
                    send(
                        mine, bundle.at[d, core, j], xbuf.at[slot_rows(i, core), col(y, q)],
                        m_ss.at[(2 * d + core) * REACH + j], z_rs.at[2 * i + core],
                        {"z": zz(way * (j + 1)), "c": 1},
                    )

        def n_send(yv, way, s):
            blk = xbuf.at[pair_rows, col2(yv)]
            k = way * LONG + s
            send(mine, blk, blk, n_ss.at[k], n_rs.at[k], toB if way else toA)

        def n_step(s):
            for way, last in ((0, LONG), (1, SHORT)):
                if s < last:
                    yv = yy(s + 1) if way else yy(-s - 1)
                    k = way * LONG + s
                    arrive(xbuf.at[pair_rows, col2(yv)], n_ss.at[k], n_rs.at[k])
                    if s < last - 1:
                        n_send(yv, way, s + 1)

        def f_send(yv, way, s):
            blk = xbuf.at[one_rows, col(yv, q)]
            k = way * LONG + s
            send(mine, blk, blk, f_ss.at[k], f_rs.at[k], toB if way else toA)

        def fx_send(yv, k):
            blk = xbuf.at[one_rows, col(yv, q)]
            send(mine, blk, blk, f_ss.at[NY + k], f_rs.at[NY + k], toN)

        def fx_arrive(yv, k):
            arrive(xbuf.at[one_rows, col(yv, 1 - q)], f_ss.at[NY + k], f_rs.at[NY + k])

        def f_step(s):
            for way, last in ((0, LONG), (1, SHORT)):
                if s < last:
                    yv = yy(s + 1) if way else yy(-s - 1)
                    k = way * LONG + s
                    arrive(xbuf.at[one_rows, col(yv, q)], f_ss.at[k], f_rs.at[k])
                    if s < last - 1:
                        f_send(yv, way, s + 1)
                    fx_send(yv, 1 + k)

        @pl.loop(DIRECT, PAIRED)
        def _(i):
            for core in range(2):
                arrive(xbuf.at[slot_rows(i, core), col2(y)], z_ss.at[i], z_rs.at[2 * i + core])

        n_send(y, 0, 0)
        n_send(y, 1, 0)

        d_step(0)
        n_step(0)

        @pl.loop(PAIRED, NZ)
        def _(i):
            for core in range(2):
                arrive(xbuf.at[slot_rows(i, core), col(y, q)], z_ss.at[i], z_rs.at[2 * i + core])

        f_send(y, 0, 0)
        f_send(y, 1, 0)
        fx_send(y, 0)
        whole_send()
        weights_of_rows()

        def experts(rows):
            halves = []
            for b in range(2):
                gu = jnp.dot(xbuf[rows, :], w1[b], preferred_element_type=F32)
                gv, uv = gu[:, :C], gu[:, C:]
                halves.append((gv * (1.0 / (1.0 + jnp.exp(-gv))) * uv).astype(BF16))
            hidden = jnp.concatenate(halves, axis=1)
            width = 512
            for n in range(D // width):
                cols = pl.ds(n * width, width)
                wdn = wd[:, :, cols].reshape(2 * C, width)
                part[rows, cols] = jnp.dot(hidden, wdn, preferred_element_type=F32).astype(BF16)

        def add(*terms):
            total = terms[0].astype(F32)
            for t in terms[1:]:
                total = total + t.astype(F32)
            return total.astype(BF16)

        def ready():
            @pl.when(g == 1)
            def _():
                for i in range(3):
                    pltpu.make_async_copy(own_w[i], w_dst(0)[i], w_rs.at[i]).wait()

            @pl.when(g == 0)
            def _():
                for i in range(3):
                    arrive(w_dst(0)[i], w_ss.at[i], w_rs.at[i])

            for i in range(3):
                arrive(w_dst(1)[i], w_ss.at[i], w_rs.at[3 + i])
            arrive(xbuf.at[slot_rows(0, 0), :], z_ss.at[0], z_rs.at[0])
            for i in range(1, DIRECT):
                for core in range(2):
                    arrive(xbuf.at[slot_rows(i, core), :], z_ss.at[i], z_rs.at[2 * i + core])

        blocks = (pl.ds(0, 2 * DIRECT * SLOT), pl.ds(2 * DIRECT * SLOT, NR - 2 * DIRECT * SLOT))

        def rn_send(src, blk, way, s):
            k = blk * NY + 1 + way * LONG + s
            dst = (nb if way else na).at[s, blocks[blk], :]
            send(mine, src, dst, rn_ss.at[k], rn_rs.at[k], toB if way else toA)

        def rn_start(blk):
            rn_send(part.at[blocks[blk], col2(yy(LONG))], blk, 0, 0)
            rn_send(part.at[blocks[blk], col2(yy(-SHORT))], blk, 1, 0)

        def rn_step(s):
            for blk, rows in enumerate(blocks):
                for way, last, buf in ((0, LONG, na), (1, SHORT, nb)):
                    if s < last:
                        k = blk * NY + 1 + way * LONG + s
                        arrive(buf.at[s, rows, :], rn_ss.at[k], rn_rs.at[k])
                        if s < last - 1:
                            j = s + 1 - SHORT if way else LONG - 1 - s
                            buf[s, rows, :] = add(buf[s, rows, :], part[rows, col2(yy(j))])
                            rn_send(buf.at[s, rows, :], blk, way, s + 1)
                if s == LONG - 1:
                    na[s, rows, :] = add(na[s, rows, :], nb[SHORT - 1, rows, :], part[rows, col2(y)])
                    k = blk * NY
                    send(
                        mine, na.at[s, rows, pl.ds(pl.multiple_of((1 - q) * C, C), C)],
                        nxr.at[rows, :], rn_ss.at[k], rn_rs.at[k], toN,
                    )

        d_step(1)
        for s in range(1, LONG):
            f_step(s - 1)
            n_step(s)
            d_step(s + 1)
            if s == max(1, LONG - 2):
                ready()
                experts(blocks[0])
                rn_start(0)
        experts(blocks[1])
        rn_start(1)
        f_step(LONG - 1)
        rn_step(0)

        for k in range(NY):
            fx_arrive(yy(-k) if k <= LONG else yy(k - LONG), k)
        experts(far)

        def rx_index(j):
            return j if j >= 0 else LONG - j

        order = [LONG]
        for j in range(SHORT, 0, -1):
            order += [-j, j]
        order += [0]
        for j in order:
            k = rx_index(j)
            send(mine, part.at[far, col(yy(j), 1 - q)], fxr.at[k], rf_ss.at[NY + k], rf_rs.at[NY + k], toN)

        def rf_send(src, way, s):
            k = way * LONG + s
            dst = fb.at[s] if way else fa.at[s]
            send(mine, src, dst, rf_ss.at[k], rf_rs.at[k], toB if way else toA)

        def rx_arrive(j):
            k = rx_index(j)
            arrive(fxr.at[k], rf_ss.at[NY + k], rf_rs.at[NY + k])
            return fxr[k], part[far, col(yy(j), q)]

        def rf_step(s):
            for way, last, buf in ((0, LONG, fa), (1, SHORT, fb)):
                if s < last:
                    k = way * LONG + s
                    if s < last - 1:
                        j = s + 1 - SHORT if way else LONG - 1 - s
                        terms = rx_arrive(j)
                    arrive(buf.at[s], rf_ss.at[k], rf_rs.at[k])
                    if s < last - 1:
                        buf[s] = add(buf[s], *terms)
                        rf_send(buf.at[s], way, s + 1)

        d_across()
        rn_step(1)
        fxr[LONG] = add(*rx_arrive(LONG))
        rf_send(fxr.at[LONG], 0, 0)
        fxr[LONG + SHORT] = add(*rx_arrive(-SHORT))
        rf_send(fxr.at[LONG + SHORT], 1, 0)

        for s in range(2, LONG):
            rn_step(s)
            rf_step(s - 2)
        rf_step(LONG - 2)

        def z_return(lo, hi):
            @pl.loop(lo, hi)
            def _(i):
                for core in range(2):
                    rc(
                        fin.at[slot_rows(i, core), :], ret.at[z], r_ss.at[2 * i + core], r_rs.at[i],
                        {"z": zz(-z_off(i)), "c": core},
                    ).start()

        for blk, rows in enumerate(blocks):
            arrive(nxr.at[rows, :], rn_ss.at[blk * NY], rn_rs.at[blk * NY])
        own_sum = na[LONG - 1, :, pl.ds(pl.multiple_of(q * C, C), C)]
        fin[near, :] = add(own_sum, nxr[...])
        z_return(1, NEAR)
        rc(fin.at[slot_rows(0, 0), :], ret.at[z], r_ss.at[0], r_rs.at[0], toS).start()
        ret[z] = fin[pl.ds(SLOT, SLOT), :]
        terms = rx_arrive(0)
        rf_step(LONG - 1)
        fin[far, :] = add(fa[LONG - 1], fb[SHORT - 1], *terms)
        z_return(NEAR, NZ)
        d_pair()

        for cp in mine:
            cp.wait_send()

    arrive(dh.at[:, xp], d_ss.at[NY], d_rs.at[NY])
    arrive(dh.at[:, NX - 1 - xp], d_ss.at[NY + 1], d_rs.at[NY + 1])
    l_dout.wait()
    dense = jnp.dot(dout[...], dh[...].reshape(NY * NX * 32, T), preferred_element_type=F32)
    dense = dense * side_gate[...]

    @pl.loop(1, NZ)
    def _(i):
        arrive(ret.at[zz(z_off(i))], r_ss.at[i], r_rs.at[i])

    back = ret[...].reshape(ROWS, C)
    first = (((0,), (0,)), ((), ()))
    routed = lax.dot_general(back, m_hi[...], first, preferred_element_type=F32) + lax.dot_general(
        back, m_lo[...], first, preferred_element_type=F32
    )
    low, high = routed[: C // 2, :], routed[C // 2 :, :]
    odd = x % 2 == 1
    exch_out[...] = jnp.where(odd, low, high)
    send(sent, exch_out, exch_in, e_ss, e_rs, toP)
    own = jnp.where(odd, high, low) + dense
    arrive(exch_in, e_ss, e_rs)
    out_ref[...] = (own + exch_in[...]).astype(BF16)

    for cp in sent:
        cp.wait_send()

    @pl.loop(1, DIRECT)
    def _(i):
        rc(sel_whole.at[0], sel_whole.at[0], z_ss.at[i], z_rs.at[i], toS).wait_send()

    @pl.loop(DIRECT, PAIRED)
    def _(i):
        rc(sel.at[0], sel.at[0], z_ss.at[i], z_rs.at[i], toS).wait_send()

    @pl.when(jnp.logical_or(g != c, c == 0))
    def _():
        for i in range(3):
            rc(own_w[i], w_dst(0)[i], w_ss.at[i], w_rs.at[i], toS).wait_send()

    @pl.when(jnp.logical_not(hub))
    def _():
        rc(sel_whole.at[0], sel_whole.at[0], z_ss.at[0], z_rs.at[0], toS).wait_send()

    @pl.when(hub)
    def _():
        rc(ret.at[0], ret.at[0], r_ss.at[0], r_rs.at[0], toS).wait_send()

        @pl.loop(2, 2 * NZ)
        def _(i):
            rc(ret.at[0], ret.at[0], r_ss.at[i], r_rs.at[0], toS).wait_send()


def per_device(sizes, split, tokens, gate, up, down, side, dout, dgate, rows, wts):
    NZ, NY = sizes
    direct, paired, near = split
    T, D = tokens.shape
    slot = rows.shape[1]
    n_rows = NZ * slot
    NR, FR = 2 * near * slot, 2 * (NZ - near) * slot
    LONG, SHORT = NY // 2, NY // 2 - 1

    any_ = pl.BlockSpec(memory_space=pl.ANY)
    vmem = pl.BlockSpec(memory_space=pltpu.VMEM)
    dma = pltpu.SemaphoreType.DMA
    return pl.pallas_call(
        functools.partial(kernel, (NZ, NY, slot) + split),
        out_shape=jax.ShapeDtypeStruct((C // 2, T), BF16),
        in_specs=[any_] * 6 + [vmem] * 3,
        out_specs=vmem,
        scratch_shapes=[
            pltpu.VMEM((T, D), BF16),
            pltpu.VMEM((32, D), BF16),
            pltpu.VMEM((64, NY * NX * 32), BF16),
            pltpu.VMEM((2, D, 2 * C), BF16),
            pltpu.VMEM((2, C, D), BF16),
            pltpu.VMEM((NZ, slot, 2 * C), BF16),
            pltpu.VMEM((direct, slot, D), BF16),
            pltpu.VMEM((2 * n_rows, D), BF16),
            pltpu.VMEM((2 * n_rows, D), BF16),
            pltpu.VMEM((n_rows, T), BF16),
            pltpu.VMEM((n_rows, T), BF16),
            pltpu.VMEM((n_rows, T), BF16),
            pltpu.VMEM((NY, NX, 32, T), BF16),
            pltpu.VMEM((2, NZ // 4, slot, C), BF16),
            pltpu.VMEM((2, 2, NZ // 4, slot, C), BF16),
            pltpu.VMEM((LONG, NR, 2 * C), BF16),
            pltpu.VMEM((SHORT, NR, 2 * C), BF16),
            pltpu.VMEM((NR, C), BF16),
            pltpu.VMEM((NY, FR, C), BF16),
            pltpu.VMEM((LONG, FR, C), BF16),
            pltpu.VMEM((SHORT, FR, C), BF16),
            pltpu.VMEM((2 * n_rows, C), BF16),
            pltpu.VMEM((NZ, slot, C), BF16),
            pltpu.VMEM((C // 2, T), F32),
            pltpu.VMEM((C // 2, T), F32),
            pltpu.VMEM((1, T), F32),
            dma((3,)),
            dma((2,)), dma((4,)), dma((NZ,)),
            dma((NZ,)), dma((2 * NZ,)),
            dma((3,)), dma((6,)),
            dma((NY,)), dma((NY,)),
            dma((2 * NY,)), dma((2 * NY,)),
            dma((NY + 2,)), dma((NY + 2,)),
            dma((2 * NY,)), dma((2 * NY,)),
            dma((2 * NY,)), dma((2 * NY,)),
            dma((2 * NZ,)), dma((NZ,)),
            dma, dma,
        ],
        compiler_params=pltpu.CompilerParams(
            collective_id=0, has_side_effects=True, vmem_limit_bytes=60 * 1024 * 1024
        ),
        name="layer",
    )(
        tokens, gate, up, down, side.T, dout.T, dgate.reshape(D // C, C), rows, wts
    ).T


def solution(mesh, sizes=(16, 8), split=(5, 9, 9)):
    NZ, NY = sizes
    torus = Mesh(mesh.devices.reshape(NZ, 2, NY, NX), ("z", "c", "y", "x"))
    EP, TP = ("z", "c"), ("y", "x")
    return jax.shard_map(
        functools.partial(per_device, sizes, split),
        mesh=torus,
        in_specs=(
            P(EP, None),
            P(EP, None, TP),
            P(EP, None, TP),
            P(EP, TP, None),
            P(None, TP),
            P(None, TP),
            P(),
            P(None, EP),
            P(None, EP),
        ),
        out_specs=P(EP, TP),
        check_vma=False,
    )
```

```python
import functools

import jax
import jax.numpy as jnp
from jax import lax
from jax.experimental import pallas as pl
from jax.experimental.pallas import tpu as pltpu
from jax.sharding import Mesh
from jax.sharding import PartitionSpec as P

MESH = pl.DeviceIdType.MESH
F32 = jnp.float32
BF16 = jnp.bfloat16
C = 128
NX = 4


def kernel(
    cfg,
    tok_hbm, gate_hbm, up_hbm, down_hbm, side_hbm, dout_hbm, dgate_ref, rows_ref, wts_ref,
    out_ref,
    tok, side, dout, w1, wd, sel, sel_whole, xbuf, part, hits, m_hi, m_lo, dh, dh_own, dense_val, dense_in, sel_far, bundle,
    na, nb, nxr, fxr, fa, fb, fin, ret, exch_out, exch_in, side_gate,
    loc_sem, go, h_ss, h_rs, l_ss, l_rs, m_ss, z_ss, z_rs, w_ss, w_rs, n_ss, n_rs, f_ss, f_rs, d_ss, d_rs,
    rn_ss, rn_rs, rf_ss, rf_rs, r_ss, r_rs, e_ss, e_rs,
):
    NZ, NY, SLOT, DIRECT, PAIRED, NEAR = cfg
    LONG, SHORT = NY // 2, NY // 2 - 1
    ROWS = NZ * SLOT
    NR, FR = 2 * NEAR * SLOT, 2 * (NZ - NEAR) * SLOT
    T, D = tok.shape

    z, c, y, x = (lax.axis_index(a) for a in ("z", "c", "y", "x"))
    q = x // 2
    xn = NX - 1 - x
    xp = x + 1 - 2 * (x % 2)
    g = ((x + 1) // 2) % 2
    hub = c == 1
    REACH = NZ // 4
    sgn = 1 - 2 * c

    def yy(j):
        return lax.rem(y + sgn * j + 2 * NY, NY)

    def zz(j):
        return lax.rem(z + j + 2 * NZ, NZ)

    def z_off(i):
        return ((i + 1) // 2) * (1 - 2 * (i % 2))

    def col(yv, qv):
        return pl.ds(pl.multiple_of(yv * 2 * C + qv * C, C), C)

    def col2(yv):
        return pl.ds(pl.multiple_of(yv * 2 * C, 2 * C), 2 * C)

    near, far = pl.ds(0, NR), pl.ds(NR, FR)
    pair_rows = pl.ds(2 * DIRECT * SLOT, 2 * (PAIRED - DIRECT) * SLOT)
    one_rows = pl.ds(2 * PAIRED * SLOT, 2 * (NZ - PAIRED) * SLOT)
    toA, toB = {"y": yy(1)}, {"y": yy(-1)}
    toN, toP, toS = {"x": xn}, {"x": xp}, {"c": 1 - c}

    def rc(src, dst, ss, rs, dev):
        return pltpu.make_async_remote_copy(
            src_ref=src, dst_ref=dst, send_sem=ss, recv_sem=rs, device_id=dev, device_id_type=MESH
        )

    sent, mine = [], []

    def send(kept, src, dst, ss, rs, dev):
        cp = rc(src, dst, ss, rs, dev)
        cp.start()
        kept.append(cp)

    def arrive(dst, ss, rs):
        rc(dst, dst, ss, rs, toS).wait_recv()

    barrier = pltpu.get_barrier_semaphore()

    def greet(dev):
        pl.semaphore_signal(barrier, inc=1, device_id=dev, device_id_type=MESH)

    for dev in (toA, toB, toN, toP, toS):
        greet(dev)

    @pl.loop(1, REACH + 1)
    def _(k):
        greet({"z": zz(k), "c": 1})
        greet({"z": zz(-k), "c": 1})

    @pl.when(hub)
    def _():
        greet({"x": xp, "c": 0})

        @pl.loop(1, REACH + 1)
        def _(k):
            greet({"z": zz(k), "c": 0})
            greet({"z": zz(-k), "c": 0})

    l_tok = pltpu.make_async_copy(tok_hbm, tok, loc_sem.at[0])
    l_side = pltpu.make_async_copy(side_hbm, side, loc_sem.at[1])
    l_dout = pltpu.make_async_copy(dout_hbm, dout, loc_sem.at[2])
    l_tok.start()
    l_side.start()
    l_dout.start()
    own_w = (gate_hbm.at[0], up_hbm.at[0], down_hbm.at[0])

    def w_dst(b):
        return (w1.at[b, :, pl.ds(0, C)], w1.at[b, :, pl.ds(C, C)], wd.at[b])

    @pl.when(jnp.logical_and(hub, g == 1))
    def _():
        for i in range(3):
            pltpu.make_async_copy(own_w[i], w_dst(0)[i], w_rs.at[i]).start()

    ids = rows_ref[pl.ds(g, NZ, stride=2), :].T
    token = lax.broadcasted_iota(jnp.int32, (SLOT, T), 1)
    for k in range(NZ):
        hits[pl.ds(k * SLOT, SLOT), :] = jnp.where(ids[:, k : k + 1] == token, 1.0, 0.0).astype(BF16)
    l_tok.wait()
    picked = jnp.dot(hits[...], tok[:, col2(y)], preferred_element_type=F32)
    sel[...] = picked.astype(BF16).reshape(NZ, SLOT, 2 * C)
    own_chunk = pl.ds(pl.multiple_of(q * C, C), C)
    for d, way in enumerate((1, -1)):
        for j in range(REACH):
            sel_far[d, j] = sel[zz(way * (REACH + 1 + j)), :, own_chunk]

    @pl.when(hub)
    def _():
        pl.semaphore_wait(barrier, 5 + 4 * REACH)

    @pl.when(jnp.logical_not(hub))
    def _():
        pl.semaphore_wait(barrier, 6 + 2 * REACH)


    def slot_rows(i, core):
        return pl.ds(pl.multiple_of((2 * i + core) * SLOT, SLOT), SLOT)

    for d, way in enumerate((1, -1)):
        send(
            sent, sel_far.at[d], bundle.at[d, c], l_ss.at[d], l_rs.at[2 * d + c],
            {"z": zz(way * REACH), "c": 1},
        )

    @pl.loop(DIRECT, PAIRED)
    def _(i):
        dest = zz(z_off(i))
        rc(
            sel.at[dest], xbuf.at[slot_rows(i, c), col2(y)], z_ss.at[i], z_rs.at[2 * i + c],
            {"z": dest, "c": 1},
        ).start()

    def w_send(b, dev):
        for i in range(3):
            rc(own_w[i], w_dst(b)[i], w_ss.at[i], w_rs.at[3 * b + i], dev).start()

    keeps = g == c

    @pl.when(jnp.logical_not(keeps))
    def _():
        w_send(1, {"x": xp, "c": 1})

    @pl.when(jnp.logical_and(keeps, jnp.logical_not(hub)))
    def _():
        w_send(0, toS)

    l_side.wait()
    transposed = (((1,), (1,)), ((), ()))
    dpre = lax.dot_general(side[...], tok[...], transposed, preferred_element_type=F32)
    dense_hidden = (dpre * (1.0 / (1.0 + jnp.exp(-dpre)))).astype(BF16)

    @pl.when(hub)
    def _():
        dh_own[...] = dense_hidden
        rc(dh_own, dh.at[1, y, x], h_ss.at[0], h_rs.at[0], toS).start()

    @pl.when(jnp.logical_not(hub))
    def _():
        dh[0, y, x] = dense_hidden

    def d_send(yv, way, s):
        k = 2 + way * LONG + s
        blk = dh.at[:, yv, x]
        send(mine, blk, blk, d_ss.at[k], d_rs.at[k], toB if way else toA)

    def d_step(s):
        for way, last in ((0, LONG), (1, SHORT)):
            if s < last:
                yv = yy(s + 1) if way else yy(-s - 1)
                k = 2 + way * LONG + s
                arrive(dh.at[:, yv, x], d_ss.at[k], d_rs.at[k])
                if s < last - 1:
                    d_send(yv, way, s + 1)

    for i in range(DIRECT):
        block = hits[pl.ds(pl.multiple_of(zz(z_off(i)) * SLOT, SLOT), SLOT), :]
        sel_whole[i] = jnp.dot(block, tok[...], preferred_element_type=F32).astype(BF16)

    def whole_send():
        for i in range(1, DIRECT):
            dest = zz(z_off(i))
            rc(
                sel_whole.at[i], xbuf.at[slot_rows(i, c), :], z_ss.at[i], z_rs.at[2 * i + c],
                {"z": dest, "c": 1},
            ).start()

    def d_column(xv, k, dev):
        send(mine, dh.at[:, :, xv], dh.at[:, :, xv], d_ss.at[k], d_rs.at[k], dev)

    def weights_of_rows():
        wts = wts_ref[pl.ds(g, NZ, stride=2), :].T
        w_hi = wts.astype(BF16).astype(F32)
        w_lo = wts - w_hi
        for k in range(NZ):
            rows = pl.ds(k * SLOT, SLOT)
            hit = hits[rows, :].astype(F32)
            m_hi[rows, :] = (hit * w_hi[:, k : k + 1]).astype(BF16)
            m_lo[rows, :] = (hit * w_lo[:, k : k + 1]).astype(BF16)
        dgate = dgate_ref[...].astype(F32)
        dgate = jnp.concatenate([dgate[k : k + 1, :] for k in range(D // C)], axis=1).astype(BF16)
        logit = lax.dot_general(dgate, tok[...], transposed, preferred_element_type=F32)
        side_gate[...] = 1.0 / (1.0 + jnp.exp(-logit))

    @pl.when(jnp.logical_not(hub))
    def _():
        mine.clear()
        rc(
            sel_whole.at[0], xbuf.at[slot_rows(0, 0), :], z_ss.at[0], z_rs.at[0], toS
        ).start()
        arrive(dh.at[1, y, x], h_ss.at[0], h_rs.at[0])
        d_send(y, 0, 0)
        d_send(y, 1, 0)
        d_step(0)
        weights_of_rows()
        for s in range(1, LONG):
            if s == LONG - 1:
                whole_send()
            d_step(s)
        d_column(x, 0, toP)
        pl.semaphore_wait(go, 1)
        d_column(x, 1, toN)
        arrive(dh.at[:, :, xn], d_ss.at[1], d_rs.at[1])
        d_column(xn, NY + 1, toP)
        l_dout.wait()
        arrive(dh.at[:, :, xp], d_ss.at[0], d_rs.at[0])
        arrive(dh.at[:, :, NX - 1 - xp], d_ss.at[NY + 1], d_rs.at[NY + 1])
        for core in (1, 0):
            dense_val[core] = jnp.dot(
                dout[...], dh[core].reshape(NY * NX * 32, T), preferred_element_type=F32
            )
            if core == 1:
                send(mine, dense_val.at[1], dense_in, h_ss.at[1], h_rs.at[1], toS)
        dense_in[...] = dense_val[0]
        arrive(ret.at[z], r_ss.at[0], r_rs.at[0])
        for cp in mine:
            cp.wait_send()

    @pl.when(hub)
    def _():
        mine.clear()
        xbuf[slot_rows(0, 1), :] = sel_whole[0]
        for d, way in enumerate((1, -1)):
            for core in range(2):
                arrive(bundle.at[d, core], l_ss.at[d], l_rs.at[2 * d + core])
                for j in range(REACH):
                    k = REACH + 1 + j
                    if 2 * k == NZ and d != core:
                        continue
                    i = 2 * k - 1 if d else min(2 * k, NZ - 1)
                    send(
                        mine, bundle.at[d, core, j], xbuf.at[slot_rows(i, core), col(y, q)],
                        m_ss.at[(2 * d + core) * REACH + j], z_rs.at[2 * i + core],
                        {"z": zz(way * (j + 1)), "c": 1},
                    )

        def n_send(yv, way, s):
            blk = xbuf.at[pair_rows, col2(yv)]
            k = way * LONG + s
            send(mine, blk, blk, n_ss.at[k], n_rs.at[k], toB if way else toA)

        def n_step(s):
            for way, last in ((0, LONG), (1, SHORT)):
                if s < last:
                    yv = yy(s + 1) if way else yy(-s - 1)
                    k = way * LONG + s
                    arrive(xbuf.at[pair_rows, col2(yv)], n_ss.at[k], n_rs.at[k])
                    if s < last - 1:
                        n_send(yv, way, s + 1)

        def f_send(yv, way, s):
            blk = xbuf.at[one_rows, col(yv, q)]
            k = way * LONG + s
            send(mine, blk, blk, f_ss.at[k], f_rs.at[k], toB if way else toA)

        def fx_send(yv, k):
            blk = xbuf.at[one_rows, col(yv, q)]
            send(mine, blk, blk, f_ss.at[NY + k], f_rs.at[NY + k], toN)

        def fx_arrive(yv, k):
            arrive(xbuf.at[one_rows, col(yv, 1 - q)], f_ss.at[NY + k], f_rs.at[NY + k])

        def f_step(s):
            for way, last in ((0, LONG), (1, SHORT)):
                if s < last:
                    yv = yy(s + 1) if way else yy(-s - 1)
                    k = way * LONG + s
                    arrive(xbuf.at[one_rows, col(yv, q)], f_ss.at[k], f_rs.at[k])
                    if s < last - 1:
                        f_send(yv, way, s + 1)
                    fx_send(yv, 1 + k)

        @pl.loop(DIRECT, PAIRED)
        def _(i):
            for core in range(2):
                arrive(xbuf.at[slot_rows(i, core), col2(y)], z_ss.at[i], z_rs.at[2 * i + core])

        n_send(y, 0, 0)
        n_send(y, 1, 0)

        @pl.loop(PAIRED, NZ)
        def _(i):
            for core in range(2):
                arrive(xbuf.at[slot_rows(i, core), col(y, q)], z_ss.at[i], z_rs.at[2 * i + core])

        f_send(y, 0, 0)
        f_send(y, 1, 0)
        fx_send(y, 0)
        whole_send()
        n_step(0)
        weights_of_rows()

        def experts(rows):
            halves = []
            for b in range(2):
                gu = jnp.dot(xbuf[rows, :], w1[b], preferred_element_type=F32)
                gv, uv = gu[:, :C], gu[:, C:]
                halves.append((gv * (1.0 / (1.0 + jnp.exp(-gv))) * uv).astype(BF16))
            hidden = jnp.concatenate(halves, axis=1)
            width = 512
            for n in range(D // width):
                cols = pl.ds(n * width, width)
                wdn = wd[:, :, cols].reshape(2 * C, width)
                part[rows, cols] = jnp.dot(hidden, wdn, preferred_element_type=F32).astype(BF16)

        def add(*terms):
            total = terms[0].astype(F32)
            for t in terms[1:]:
                total = total + t.astype(F32)
            return total.astype(BF16)

        def ready():
            @pl.when(g == 1)
            def _():
                for i in range(3):
                    pltpu.make_async_copy(own_w[i], w_dst(0)[i], w_rs.at[i]).wait()

            @pl.when(g == 0)
            def _():
                for i in range(3):
                    arrive(w_dst(0)[i], w_ss.at[i], w_rs.at[i])

            for i in range(3):
                arrive(w_dst(1)[i], w_ss.at[i], w_rs.at[3 + i])
            arrive(xbuf.at[slot_rows(0, 0), :], z_ss.at[0], z_rs.at[0])
            for i in range(1, DIRECT):
                for core in range(2):
                    arrive(xbuf.at[slot_rows(i, core), :], z_ss.at[i], z_rs.at[2 * i + core])

        blocks = (pl.ds(0, 2 * DIRECT * SLOT), pl.ds(2 * DIRECT * SLOT, NR - 2 * DIRECT * SLOT))

        def rn_send(src, blk, way, s):
            k = blk * NY + 1 + way * LONG + s
            dst = (nb if way else na).at[s, blocks[blk], :]
            send(mine, src, dst, rn_ss.at[k], rn_rs.at[k], toB if way else toA)

        def rn_start(blk):
            rn_send(part.at[blocks[blk], col2(yy(LONG))], blk, 0, 0)
            rn_send(part.at[blocks[blk], col2(yy(-SHORT))], blk, 1, 0)

        def rn_step(blk, s):
            for rows in blocks[blk : blk + 1]:
                for way, last, buf in ((0, LONG, na), (1, SHORT, nb)):
                    if s < last:
                        k = blk * NY + 1 + way * LONG + s
                        arrive(buf.at[s, rows, :], rn_ss.at[k], rn_rs.at[k])
                        if s < last - 1:
                            j = s + 1 - SHORT if way else LONG - 1 - s
                            buf[s, rows, :] = add(buf[s, rows, :], part[rows, col2(yy(j))])
                            rn_send(buf.at[s, rows, :], blk, way, s + 1)
                if s == LONG - 1:
                    na[s, rows, :] = add(na[s, rows, :], nb[SHORT - 1, rows, :], part[rows, col2(y)])
                    k = blk * NY
                    send(
                        mine, na.at[s, rows, pl.ds(pl.multiple_of((1 - q) * C, C), C)],
                        nxr.at[rows, :], rn_ss.at[k], rn_rs.at[k], toN,
                    )

        for s in range(LONG):
            f_step(s)
            if s == 1 and LONG > 2:
                n_step(1)
            if s == LONG - 2:
                ready()
                experts(blocks[0])
                rn_start(0)
                for k in range(2, LONG - 1):
                    n_step(k)
        rn_step(0, 0)

        for k in range(NY):
            fx_arrive(yy(-k) if k <= LONG else yy(k - LONG), k)
        experts(far)

        def rx_index(j):
            return j if j >= 0 else LONG - j

        order = [LONG]
        for j in range(SHORT, 0, -1):
            order += [-j, j]
        order += [0]
        for j in order:
            k = rx_index(j)
            send(mine, part.at[far, col(yy(j), 1 - q)], fxr.at[k], rf_ss.at[NY + k], rf_rs.at[NY + k], toN)

        def rf_send(src, way, s):
            k = way * LONG + s
            dst = fb.at[s] if way else fa.at[s]
            send(mine, src, dst, rf_ss.at[k], rf_rs.at[k], toB if way else toA)

        def rx_arrive(j):
            k = rx_index(j)
            arrive(fxr.at[k], rf_ss.at[NY + k], rf_rs.at[NY + k])
            return fxr[k], part[far, col(yy(j), q)]

        def rf_step(s):
            for way, last, buf in ((0, LONG, fa), (1, SHORT, fb)):
                if s < last:
                    k = way * LONG + s
                    if s < last - 1:
                        j = s + 1 - SHORT if way else LONG - 1 - s
                        terms = rx_arrive(j)
                    arrive(buf.at[s], rf_ss.at[k], rf_rs.at[k])
                    if s < last - 1:
                        buf[s] = add(buf[s], *terms)
                        rf_send(buf.at[s], way, s + 1)

        n_step(LONG - 1)
        experts(blocks[1])
        rn_start(1)
        rn_step(0, 1)
        fxr[LONG] = add(*rx_arrive(LONG))
        rf_send(fxr.at[LONG], 0, 0)
        fxr[LONG + SHORT] = add(*rx_arrive(-SHORT))
        rf_send(fxr.at[LONG + SHORT], 1, 0)
        rn_step(1, 0)
        if LONG > 2:
            rn_step(0, 2)
        for s in range(LONG - 1):
            rf_step(s)
            if s == 0:
                pl.semaphore_signal(go, inc=1, device_id=toS, device_id_type=MESH)
            if s == 1 and LONG > 3:
                rn_step(0, 3)
            if s + 1 < LONG - 1:
                rn_step(1, s + 1)

        def z_return(lo, hi):
            @pl.loop(0, hi - lo)
            def _(back):
                i = hi - 1 - back
                for core in range(2):
                    rc(
                        fin.at[slot_rows(i, core), :], ret.at[z], r_ss.at[2 * i + core], r_rs.at[i],
                        {"z": zz(-z_off(i)), "c": core},
                    ).start()

        terms = rx_arrive(0)
        rf_step(LONG - 1)
        fin[far, :] = add(fa[LONG - 1], fb[SHORT - 1], *terms)
        z_return(NEAR, NZ)
        for blk, (lo, hi) in enumerate(((0, DIRECT), (DIRECT, NEAR))):
            rows = blocks[blk]
            if blk == 1:
                rn_step(1, LONG - 1)
            arrive(nxr.at[rows, :], rn_ss.at[blk * NY], rn_rs.at[blk * NY])
            own_sum = na[LONG - 1, rows, pl.ds(pl.multiple_of(q * C, C), C)]
            fin[rows, :] = add(own_sum, nxr[rows, :])
            z_return(max(lo, 1), hi)
        rc(fin.at[slot_rows(0, 0), :], ret.at[z], r_ss.at[0], r_rs.at[0], toS).start()
        ret[z] = fin[pl.ds(SLOT, SLOT), :]
        l_dout.wait()
        arrive(dense_in, h_ss.at[1], h_rs.at[1])
        rc(dh_own, dh_own, h_ss.at[0], h_rs.at[0], toS).wait_send()
        for cp in mine:
            cp.wait_send()

    @pl.loop(1, NZ)
    def _(i):
        arrive(ret.at[zz(z_off(i))], r_ss.at[i], r_rs.at[i])

    back = ret[...].reshape(ROWS, C)
    first = (((0,), (0,)), ((), ()))
    routed = lax.dot_general(back, m_hi[...], first, preferred_element_type=F32) + lax.dot_general(
        back, m_lo[...], first, preferred_element_type=F32
    )
    low, high = routed[: C // 2, :], routed[C // 2 :, :]
    odd = x % 2 == 1
    exch_out[...] = jnp.where(odd, low, high).astype(BF16)
    send(sent, exch_out, exch_in, e_ss, e_rs, toP)
    own = jnp.where(odd, high, low) + dense_in[...] * side_gate[...]
    arrive(exch_in, e_ss, e_rs)
    out_ref[...] = (own + exch_in[...].astype(F32)).astype(BF16)

    for cp in sent:
        cp.wait_send()

    @pl.loop(1, DIRECT)
    def _(i):
        rc(sel_whole.at[0], sel_whole.at[0], z_ss.at[i], z_rs.at[i], toS).wait_send()

    @pl.loop(DIRECT, PAIRED)
    def _(i):
        rc(sel.at[0], sel.at[0], z_ss.at[i], z_rs.at[i], toS).wait_send()

    @pl.when(jnp.logical_or(g != c, c == 0))
    def _():
        for i in range(3):
            rc(own_w[i], w_dst(0)[i], w_ss.at[i], w_rs.at[i], toS).wait_send()

    @pl.when(jnp.logical_not(hub))
    def _():
        rc(sel_whole.at[0], sel_whole.at[0], z_ss.at[0], z_rs.at[0], toS).wait_send()

    @pl.when(hub)
    def _():
        rc(ret.at[0], ret.at[0], r_ss.at[0], r_rs.at[0], toS).wait_send()

        @pl.loop(2, 2 * NZ)
        def _(i):
            rc(ret.at[0], ret.at[0], r_ss.at[i], r_rs.at[0], toS).wait_send()


def per_device(sizes, split, tokens, gate, up, down, side, dout, dgate, rows, wts):
    NZ, NY = sizes
    direct, paired, near = split
    T, D = tokens.shape
    slot = rows.shape[1]
    n_rows = NZ * slot
    NR, FR = 2 * near * slot, 2 * (NZ - near) * slot
    LONG, SHORT = NY // 2, NY // 2 - 1

    any_ = pl.BlockSpec(memory_space=pl.ANY)
    vmem = pl.BlockSpec(memory_space=pltpu.VMEM)
    dma = pltpu.SemaphoreType.DMA
    return pl.pallas_call(
        functools.partial(kernel, (NZ, NY, slot) + split),
        out_shape=jax.ShapeDtypeStruct((C // 2, T), BF16),
        in_specs=[any_] * 6 + [vmem] * 3,
        out_specs=vmem,
        scratch_shapes=[
            pltpu.VMEM((T, D), BF16),
            pltpu.VMEM((32, D), BF16),
            pltpu.VMEM((64, NY * NX * 32), BF16),
            pltpu.VMEM((2, D, 2 * C), BF16),
            pltpu.VMEM((2, C, D), BF16),
            pltpu.VMEM((NZ, slot, 2 * C), BF16),
            pltpu.VMEM((direct, slot, D), BF16),
            pltpu.VMEM((2 * n_rows, D), BF16),
            pltpu.VMEM((2 * n_rows, D), BF16),
            pltpu.VMEM((n_rows, T), BF16),
            pltpu.VMEM((n_rows, T), BF16),
            pltpu.VMEM((n_rows, T), BF16),
            pltpu.VMEM((2, NY, NX, 32, T), BF16),
            pltpu.VMEM((32, T), BF16),
            pltpu.VMEM((2, C // 2, T), F32),
            pltpu.VMEM((C // 2, T), F32),
            pltpu.VMEM((2, NZ // 4, slot, C), BF16),
            pltpu.VMEM((2, 2, NZ // 4, slot, C), BF16),
            pltpu.VMEM((LONG, NR, 2 * C), BF16),
            pltpu.VMEM((SHORT, NR, 2 * C), BF16),
            pltpu.VMEM((NR, C), BF16),
            pltpu.VMEM((NY, FR, C), BF16),
            pltpu.VMEM((LONG, FR, C), BF16),
            pltpu.VMEM((SHORT, FR, C), BF16),
            pltpu.VMEM((2 * n_rows, C), BF16),
            pltpu.VMEM((NZ, slot, C), BF16),
            pltpu.VMEM((C // 2, T), BF16),
            pltpu.VMEM((C // 2, T), BF16),
            pltpu.VMEM((1, T), F32),
            dma((3,)),
            pltpu.SemaphoreType.REGULAR, dma((2,)), dma((2,)),
            dma((2,)), dma((4,)), dma((NZ,)),
            dma((NZ,)), dma((2 * NZ,)),
            dma((3,)), dma((6,)),
            dma((NY,)), dma((NY,)),
            dma((2 * NY,)), dma((2 * NY,)),
            dma((NY + 2,)), dma((NY + 2,)),
            dma((2 * NY,)), dma((2 * NY,)),
            dma((2 * NY,)), dma((2 * NY,)),
            dma((2 * NZ,)), dma((NZ,)),
            dma, dma,
        ],
        compiler_params=pltpu.CompilerParams(
            collective_id=0, has_side_effects=True, vmem_limit_bytes=60 * 1024 * 1024
        ),
        name="layer",
    )(
        tokens, gate, up, down, side.T, dout.T, dgate.reshape(D // C, C), rows, wts
    ).T


def solution(mesh, sizes=(16, 8), split=(5, 9, 9)):
    NZ, NY = sizes
    torus = Mesh(mesh.devices.reshape(NZ, 2, NY, NX), ("z", "c", "y", "x"))
    EP, TP = ("z", "c"), ("y", "x")
    return jax.shard_map(
        functools.partial(per_device, sizes, split),
        mesh=torus,
        in_specs=(
            P(EP, None),
            P(EP, None, TP),
            P(EP, None, TP),
            P(EP, TP, None),
            P(None, TP),
            P(None, TP),
            P(),
            P(None, EP),
            P(None, EP),
        ),
        out_specs=P(EP, TP),
        check_vma=False,
    )
```
